32 devices in a mesh: kv: 4 (over y, x), tp: 8 (over z, core).
Axes of the slice: x: 2, y: 2, z: 4, core: 2. Of those that a mesh axis runs over, the one named last changes fastest.
Arguments:
- stream: bfloat16 [32, 4096], P(None, ('kv', 'tp')), may hold values from -18 to 18
- mixer_gain: float32 [4096], replicated, may hold values from 0.1 to 1.9
- query_weight: bfloat16 [4096, 1024], P(None, 'tp'), may hold values from -0.09375 to 0.09375
- key_weight: bfloat16 [4096, 1024], P(None, 'tp'), may hold values from -0.09375 to 0.09375
- value_weight: bfloat16 [4096, 1024], P(None, 'tp'), may hold values from -0.09375 to 0.09375
- forget_weight: bfloat16 [4096, 16], replicated, may hold values from -0.09375 to 0.09375
- forget_bias: float32 [16], replicated, may hold values from -4 to -2
- key_cache: bfloat16 [32, 16, 4096, 64], P(None, 'tp', 'kv'), may hold values from -512 to 512, as said below
- value_cache: bfloat16 [32, 16, 4096, 64], P(None, 'tp', 'kv'), may hold values from -12 to 12
- past_decay: float32 [32, 16, 4096], P(None, 'tp', 'kv'), may hold values from -4096 to 0, as said below
- out_weight: bfloat16 [1024, 4096], P('tp', 'kv'), may hold values from -0.75 to 0.75
- channel_gain: float32 [4096], replicated, may hold values from 0.1 to 1.9
- up_weight: bfloat16 [4096, 16384], P('kv', 'tp'), may hold values from -0.09375 to 0.09375
- down_weight: bfloat16 [16384, 4096], P('tp', 'kv'), may hold values from -0.0625 to 0.0625
Outputs:
- updated: bfloat16 [32, 4096], P(None, ('kv', 'tp'))
The draws below stay inside these ranges and needn't reach their ends.
Inputs may be any that keep to these rules, and one draw needn't show every extreme that they name: `key_cache`: keys of order one; some cached keys may be much larger. `past_decay`: never falling along the positions of a sequence and head, zero at the last cached position.
All inputs are finite; a program needn't handle non-finite values.
Results may differ from the reference program's by a relative error of at most 0.014.
The reference program's roundings to bfloat16 on the way count: a program that leaves them out, or rounds other values in their place, can miss the bound.
Values may be sent and summed in bfloat16 or wider, within the bound.
A program may use at most 64 MiB of HBM per device.

```python
import math
import jax
import jax.numpy as jnp
from jax import lax

D = 4096
HEADS = 16
HEAD = 64
FF = 16384
BATCH = 32
POS_DEV = 1024
BLOCK = 256
CACHE = 4096


def draw_stream(key, part):
    first_key = jax.random.fold_in(jax.random.fold_in(key, 5), 0)
    columns = jnp.exp(jnp.linspace(0.0, math.log(3.0), D).astype(jnp.float32))
    base = jax.random.normal(first_key, (BATCH, D), jnp.float32)
    values = jnp.clip(base, -6.0, 6.0) * columns[None, :]
    return values.astype(jnp.bfloat16)


def draw_key_cache(key, part):
    first_key = jax.random.fold_in(jax.random.fold_in(key, 11), 0)
    values = 2.0 * jax.random.normal(first_key, (BATCH, HEADS, CACHE, HEAD), jnp.float32)
    values = jnp.clip(values, -12.0, 12.0)
    return values.astype(jnp.bfloat16)


def draw_value_cache(key, part):
    first_key, offset_key = jax.random.split(jax.random.fold_in(key, 23), 2)
    base = jax.random.normal(first_key, (BATCH, HEADS, CACHE, HEAD), jnp.float32)
    offsets = jax.random.normal(offset_key, (BATCH, HEADS, CACHE // BLOCK, 1, HEAD), jnp.float32)
    offsets = jnp.broadcast_to(offsets, (BATCH, HEADS, CACHE // BLOCK, BLOCK, HEAD)).reshape(BATCH, HEADS, CACHE, HEAD)
    return jnp.clip(base + offsets, -12.0, 12.0).astype(jnp.bfloat16)


def draw_past_decay(key, part):
    pick_key, rate_key, block_key, rough_key = jax.random.split(jax.random.fold_in(key, 37), 4)
    fast = jax.random.uniform(pick_key, (1, HEADS, 1)) < 0.5
    fast_rate = jnp.exp(jax.random.uniform(rate_key, (1, HEADS, 1), jnp.float32, math.log(1.0 / 30.0), math.log(1.0 / 12.0)))
    rate = jnp.where(fast, fast_rate, 0.5 / CACHE)
    block_factor = jnp.exp(jax.random.uniform(block_key, (BATCH, HEADS, CACHE // BLOCK, 1), jnp.float32, -math.log(4.0), math.log(4.0)))
    block_factor = jnp.broadcast_to(block_factor, (BATCH, HEADS, CACHE // BLOCK, BLOCK)).reshape(BATCH, HEADS, CACHE)
    rough = jnp.exp(jax.random.uniform(rough_key, (BATCH, HEADS, CACHE), jnp.float32, -math.log(2.0), math.log(2.0)))
    log_gates = -rate * block_factor * rough
    after = jnp.flip(jnp.cumsum(jnp.flip(log_gates, -1), -1), -1) - log_gates
    return jnp.clip(after, -1.0 * CACHE, 0.0)


def strengthened(values, rng, source, target, parts, factor):
    owner, partner = [(jnp.arange(values.shape[position]) // (values.shape[position] // parts)).reshape([-1 if axis == position else 1 for axis in range(values.ndim)]) for position in (source, target)]
    chosen = jax.random.permutation(rng, parts)[partner]
    strong = (owner == chosen) | (owner == (partner + parts // 2) % parts)
    return jnp.where(strong, factor * values, values)


def block_levels(stream_key, dims, shards, least, high):
    def one(dim, parts):
        heights = jax.random.uniform(jax.random.fold_in(jax.random.fold_in(stream_key, 6), dim), (parts,), jnp.float32, least / len(shards), high / len(shards))
        return jnp.repeat(jnp.exp(heights), dims[dim] // parts).reshape((-1,) + (1,) * (len(dims) - dim - 1))

    level = one(*shards[0])
    for cut in shards[1:]:
        level = level * one(*cut)
    return level


def normal_values(rng, dims, deviation, reach, cuts=(), held_as=jnp.bfloat16):
    array = deviation * jax.random.normal(rng, dims, jnp.float32)
    if cuts:
        array = array * block_levels(rng, dims, cuts, -0.22, 0.18)
    return jnp.clip(array, -reach, reach).astype(held_as)


def noise_with(rng, dims, deviation, bound, cuts, heavy, held_as=jnp.bfloat16):
    entries = deviation * jax.random.normal(rng, dims, jnp.float32)
    if cuts:
        entries = entries * block_levels(rng, dims, cuts, -0.22, 0.18)
    return jnp.clip(strengthened(entries, jax.random.fold_in(rng, 3), *heavy), -bound, bound).astype(held_as)


def setup_inputs(seed: int = 0) -> dict:
    streams_of = jax.random.split(jax.random.key(seed), 15)
    return {
        "stream": draw_stream(jax.random.fold_in(streams_of[14], 71), 0),
        "mixer_gain": jnp.clip(1.0 + 0.18 * jax.random.normal(streams_of[1], (D,), jnp.float32), 0.1, 1.9),
        "query_weight": normal_values(streams_of[2], (D, HEADS * HEAD), D ** -0.5, 0.09375, ((1, 8),)),
        "key_weight": normal_values(streams_of[3], (D, HEADS * HEAD), D ** -0.5, 0.09375, ((1, 8),)),
        "value_weight": normal_values(streams_of[4], (D, HEADS * HEAD), D ** -0.5, 0.09375, ((1, 8),)),
        "forget_weight": normal_values(streams_of[5], (D, HEADS), D ** -0.5, 0.09375),
        "forget_bias": jnp.clip(jax.random.uniform(streams_of[6], (HEADS,), jnp.float32, -4.0, -2.0), -4.0, -2.0),
        "key_cache": draw_key_cache(jax.random.fold_in(streams_of[14], 71), 0),
        "value_cache": draw_value_cache(jax.random.fold_in(streams_of[14], 71), 0),
        "past_decay": draw_past_decay(jax.random.fold_in(streams_of[14], 71), 0),
        "out_weight": noise_with(streams_of[10], (HEADS * HEAD, D), (HEADS * HEAD // 8) ** -0.5, 0.75, ((0, 8), (1, 4)), (0, 1, 8, 2.0)),
        "channel_gain": jnp.clip(1.0 + 0.18 * jax.random.normal(streams_of[11], (D,), jnp.float32), 0.1, 1.9),
        "up_weight": normal_values(streams_of[12], (D, FF), D ** -0.5, 0.09375, ((0, 4), (1, 8))),
        "down_weight": noise_with(streams_of[13], (FF, D), FF ** -0.5, 0.0625, ((0, 8), (1, 4)), (0, 1, 8, 2.0)),
    }


EPS = 1e-06

def rms_scale(values, gain):
    widened = values.astype(jnp.float32)
    inverse = lax.rsqrt(lax.optimization_barrier(jnp.mean(widened * widened, axis=-1, keepdims=True)) + EPS)
    return (widened * inverse * gain.astype(jnp.float32)).astype(jnp.bfloat16)

def reference(stream, mixer_gain, query_weight, key_weight, value_weight, forget_weight, forget_bias, key_cache, value_cache, past_decay, out_weight, channel_gain, up_weight, down_weight):
    scale_factor = float(HEAD) ** (-0.5)
    normed = rms_scale(stream, mixer_gain)
    queries = jnp.dot(normed, query_weight, preferred_element_type=jnp.float32).astype(jnp.bfloat16)
    keys_new = jnp.dot(normed, key_weight, preferred_element_type=jnp.float32).astype(jnp.bfloat16)
    values_new = jnp.dot(normed, value_weight, preferred_element_type=jnp.float32).astype(jnp.bfloat16)
    forget = jax.nn.log_sigmoid(jnp.dot(normed, forget_weight, preferred_element_type=jnp.float32) + forget_bias.astype(jnp.float32))
    query_heads = queries.reshape(BATCH, HEADS, HEAD).astype(jnp.float32)
    key_heads = keys_new.reshape(BATCH, HEADS, HEAD).astype(jnp.float32)
    value_heads = values_new.reshape(BATCH, HEADS, HEAD).astype(jnp.float32)
    block_count = CACHE // POS_DEV

    def per_head(index):
        keys = lax.dynamic_index_in_dim(key_cache, index, 1, keepdims=False).astype(jnp.float32)
        values = lax.dynamic_index_in_dim(value_cache, index, 1, keepdims=False).astype(jnp.float32)
        decay = lax.dynamic_index_in_dim(past_decay, index, 1, keepdims=False).astype(jnp.float32)
        query_one = lax.dynamic_index_in_dim(query_heads, index, 1, keepdims=False)
        forget_one = lax.dynamic_index_in_dim(forget, index, 1, keepdims=False)
        scores = jnp.einsum('bd,bpd->bp', query_one, keys) * scale_factor + forget_one[:, None] + decay
        scores = scores.reshape(BATCH, block_count, POS_DEV)
        tops = lax.optimization_barrier(jnp.max(scores, axis=-1))
        weights = jnp.exp(scores - tops[..., None]).astype(jnp.bfloat16)
        weights = lax.optimization_barrier(weights).astype(jnp.float32)
        totals = lax.optimization_barrier(jnp.sum(weights, axis=-1))
        sums = jnp.einsum('bnp,bnpd->bnd', weights, values.reshape(BATCH, block_count, POS_DEV, HEAD))
        return (tops, totals, sums)
    tops, totals, sums = lax.map(per_head, jnp.arange(HEADS).astype(jnp.int32))
    own = (lax.optimization_barrier(jnp.sum(query_heads * key_heads, axis=-1)) * scale_factor).T
    peak = jnp.maximum(lax.optimization_barrier(jnp.max(tops, axis=-1)), own)
    factors = jnp.exp(tops - peak[..., None])
    own_factor = jnp.exp(own - peak)
    numer = lax.optimization_barrier(jnp.sum(sums * factors[..., None], axis=2)) + jnp.transpose(value_heads, (1, 0, 2)) * own_factor[..., None]
    denom = lax.optimization_barrier(jnp.sum(totals * factors, axis=-1)) + own_factor
    attention = jnp.transpose(numer / denom[..., None], (1, 0, 2)).reshape(BATCH, HEADS * HEAD).astype(jnp.bfloat16)
    middle = (stream.astype(jnp.float32) + jnp.dot(attention, out_weight, preferred_element_type=jnp.float32)).astype(jnp.bfloat16)
    mixed = rms_scale(middle, channel_gain)
    hidden = jnp.square(jax.nn.relu(jnp.dot(mixed, up_weight, preferred_element_type=jnp.float32))).astype(jnp.bfloat16)
    return (middle.astype(jnp.float32) + jnp.dot(hidden, down_weight, preferred_element_type=jnp.float32)).astype(jnp.bfloat16)
```

```python
import functools

import jax
import jax.numpy as jnp
from jax import lax
from jax.experimental import pallas as pl
from jax.experimental.pallas import tpu as pltpu
from jax.sharding import PartitionSpec as P

D = 4096


EPS = 1e-06


def combined_all(part, axis, combine):
    gathered = jax.tree.map(lambda a: lax.all_gather(a, axis), part)

    def take(source):
        return jax.tree.map(lambda a: lax.dynamic_index_in_dim(a, source, 0, False), gathered)

    return lax.fori_loop(
        1, lax.axis_size(axis), lambda source, state: combine(state, take(source)), take(0)
    )


def rms_scale(values, gain):
    widened = values.astype(jnp.float32)
    inverse = lax.rsqrt(jnp.mean(widened * widened, axis=-1, keepdims=True) + EPS)
    return (widened * inverse * gain).astype(jnp.bfloat16)


def merge_parts(earlier, later):
    top_one, total_one, sums_one = earlier
    top_two, total_two, sums_two = later
    highest = jnp.maximum(top_one, top_two)
    factor_one = jnp.exp(top_one - highest)
    factor_two = jnp.exp(top_two - highest)
    return (
        highest,
        total_one * factor_one + total_two * factor_two,
        sums_one * factor_one[..., None] + sums_two * factor_two[..., None],
    )


def squared_relu(values):
    return jnp.square(jax.nn.relu(values)).astype(jnp.bfloat16)


def row_squares(values):
    widened = values.astype(jnp.float32)
    return jnp.sum(widened * widened, axis=1)


def shards(
    stream,
    mixer_gain,
    query_weight,
    key_weight,
    value_weight,
    forget_weight,
    forget_bias,
    key_cache,
    value_cache,
    past_decay,
    out_weight,
    channel_gain,
    up_weight,
    down_weight,
):
    batch_rows = stream.shape[0]
    local_heads = key_cache.shape[1]
    head_size = key_cache.shape[3]
    scale_factor = float(head_size) ** (-0.5)
    gathered = lax.all_gather(stream, ("kv", "tp"), axis=1, tiled=True)
    normed = rms_scale(gathered, mixer_gain)
    queries = jnp.dot(normed, query_weight, preferred_element_type=jnp.float32).astype(jnp.bfloat16)
    keys_new = jnp.dot(normed, key_weight, preferred_element_type=jnp.float32).astype(jnp.bfloat16)
    values_new = jnp.dot(normed, value_weight, preferred_element_type=jnp.float32).astype(
        jnp.bfloat16
    )
    forget_all = jax.nn.log_sigmoid(
        jnp.dot(normed, forget_weight, preferred_element_type=jnp.float32) + forget_bias
    )
    forget = lax.dynamic_slice_in_dim(
        forget_all, lax.axis_index("tp") * local_heads, local_heads, 1
    )
    query_heads = queries.reshape(batch_rows, local_heads, head_size)
    scores = (
        jnp.einsum("bhd,bhpd->bhp", query_heads, key_cache, preferred_element_type=jnp.float32)
        * scale_factor
        + forget[..., None]
        + past_decay
    )
    highest = jnp.max(scores, axis=-1)
    weights = jnp.exp(scores - highest[..., None]).astype(jnp.bfloat16)
    totals = jnp.sum(weights.astype(jnp.float32), axis=-1)
    sums = jnp.einsum("bhp,bhpd->bhd", weights, value_cache, preferred_element_type=jnp.float32)
    highest, totals, sums = combined_all((highest, totals, sums), "kv", merge_parts)
    key_heads = keys_new.reshape(batch_rows, local_heads, head_size).astype(jnp.float32)
    value_heads = values_new.reshape(batch_rows, local_heads, head_size).astype(jnp.float32)
    own = jnp.sum(query_heads.astype(jnp.float32) * key_heads, axis=-1) * scale_factor
    peak = jnp.maximum(highest, own)
    cache_factor = jnp.exp(highest - peak)
    own_factor = jnp.exp(own - peak)
    numer = sums * cache_factor[..., None] + value_heads * own_factor[..., None]
    denom = totals * cache_factor + own_factor
    attention = (
        (numer / denom[..., None]).astype(jnp.bfloat16).reshape(batch_rows, local_heads * head_size)
    )
    partial_value = jnp.dot(attention, out_weight, preferred_element_type=jnp.float32)
    piece_width = stream.shape[1]
    block_width = partial_value.shape[1]
    block_sum = lax.psum(partial_value, "tp")
    own_block = lax.dynamic_slice_in_dim(
        gathered, lax.axis_index("kv") * block_width, block_width, 1
    )
    middle_block = (own_block.astype(jnp.float32) + block_sum).astype(jnp.bfloat16)
    squares = lax.psum(row_squares(middle_block), "kv")
    middle_piece = lax.dynamic_slice_in_dim(
        middle_block, lax.axis_index("tp") * piece_width, piece_width, 1
    )
    inverse = lax.rsqrt(squares / D + EPS)
    gain_block = lax.dynamic_slice_in_dim(
        channel_gain, lax.axis_index("kv") * block_width, block_width, 0
    )
    mixed_block = (
        middle_block.astype(jnp.float32) * inverse[:, None] * gain_block[None, :]
    ).astype(jnp.bfloat16)
    up_partial = jnp.dot(mixed_block, up_weight, preferred_element_type=jnp.float32)
    hidden = squared_relu(lax.psum(up_partial, "kv"))
    down_partial = jnp.dot(hidden, down_weight, preferred_element_type=jnp.float32)
    reduced = lax.psum_scatter(down_partial, "tp", scatter_dimension=1, tiled=True)
    return (middle_piece.astype(jnp.float32) + reduced).astype(jnp.bfloat16)


MESH = pl.DeviceIdType.MESH
F32 = jnp.float32
BF16 = jnp.bfloat16
NT = (((1,), (1,)), ((), ()))


def layer_kernel(
    sizes,
    stream_hbm,
    mixer_gain,
    query_hbm,
    key_hbm,
    value_hbm,
    forget_weight,
    forget_bias,
    keys_hbm,
    values_hbm,
    decay_hbm,
    out_hbm,
    channel_gain,
    up_hbm,
    down_hbm,
    result,
    pieces,
    qkv_v,
    keys_v,
    values_v,
    decay_v,
    out_v,
    up_v,
    down_v,
    normed,
    query_s,
    forget_s,
    parts,
    out_parts,
    out_got,
    middles,
    mixed,
    squares,
    up_parts,
    up_got,
    hidden,
    down_sum,
    down_parts,
    down_got,
    local_sem,
    keys_sem,
    values_sem,
    tp_send,
    tp_recv,
    kv_send,
    kv_recv,
):
    n_kv, n_tp, rows, width, chunk, heads, head = sizes
    me_kv, me_tp = lax.axis_index("kv"), lax.axis_index("tp")
    groups = rows // 8
    group_depth = 8 * width
    full = n_kv * n_tp * width
    scale = float(head) ** (-0.5)

    def tp_peer(step):
        return lax.rem(me_tp + step, n_tp)

    def kv_peer(step):
        return lax.rem(me_kv + step, n_kv)

    local = []

    def load(source, target):
        copy = pltpu.make_async_copy(source, target, local_sem.at[len(local)])
        copy.start()
        local.append(copy)
        return copy

    own_in = load(stream_hbm, pieces.at[me_kv, me_tp])
    for step in range(1, n_tp):
        pl.semaphore_signal(
            pltpu.get_barrier_semaphore(), inc=1, device_id={"tp": tp_peer(step)}, device_id_type=MESH
        )
    for step in range(1, n_kv):
        pl.semaphore_signal(
            pltpu.get_barrier_semaphore(), inc=1, device_id={"kv": kv_peer(step)}, device_id_type=MESH
        )
    qkv_in = [
        load(source, qkv_v.at[:, pl.ds(at * width, width)])
        for at, source in enumerate((query_hbm, key_hbm, value_hbm))
    ]
    decay_in = load(decay_hbm, decay_v)

    def keys_copy(group):
        span = pl.ds(pl.multiple_of(group * group_depth, group_depth), group_depth)
        return pltpu.make_async_copy(keys_hbm.at[span], keys_v.at[span], keys_sem.at[group])

    def values_copy(group):
        span = pl.ds(pl.multiple_of(group * group_depth, group_depth), group_depth)
        return pltpu.make_async_copy(values_hbm.at[span], values_v.at[span], values_sem.at[group])

    for group in range(groups):
        keys_copy(group).start()
        values_copy(group).start()
    out_in = load(out_hbm, out_v)
    up_in = load(up_hbm, up_v)
    down_in = load(down_hbm, down_v)

    sent = []

    def send_tp(phase, step, source, target):
        copy = pltpu.make_async_remote_copy(
            src_ref=source,
            dst_ref=target,
            send_sem=tp_send.at[phase, step - 1],
            recv_sem=tp_recv.at[phase, step - 1],
            device_id={"tp": tp_peer(step)},
            device_id_type=MESH,
        )
        copy.start()
        sent.append(copy)
        return copy

    def send_kv(phase, step, source, target):
        copy = pltpu.make_async_remote_copy(
            src_ref=source,
            dst_ref=target,
            send_sem=kv_send.at[phase, step - 1],
            recv_sem=kv_recv.at[phase, step - 1],
            device_id={"kv": kv_peer(step)},
            device_id_type=MESH,
        )
        copy.start()
        sent.append(copy)
        return copy

    def arrive(copies):
        for copy in copies:
            copy.wait_recv()

    tp_order = sorted(range(1, n_tp), key=lambda step: -min(step, n_tp - step))
    kv_order = sorted(range(1, n_kv), key=lambda step: -step)

    own_in.wait()
    pl.semaphore_wait(pltpu.get_barrier_semaphore(), n_tp - 1 + n_kv - 1)

    mine = pieces.at[me_kv, me_tp]
    arrive([send_tp(0, step, mine, mine) for step in tp_order])
    arrive([send_kv(0, step, pieces.at[me_kv], pieces.at[me_kv]) for step in kv_order])

    total = jnp.zeros((rows, width), F32)
    for block in range(n_kv):
        for piece in range(n_tp):
            wide = pieces[block, piece].astype(F32)
            total += wide * wide
    inverse = lax.rsqrt(jnp.sum(total, axis=1, keepdims=True) / full + EPS)
    for block in range(n_kv):
        for piece in range(n_tp):
            at = block * n_tp + piece
            wide = pieces[block, piece].astype(F32)
            normed[:, at * width : (at + 1) * width] = (
                wide * inverse * mixer_gain[at : at + 1, :]
            ).astype(BF16)

    logits = (
        lax.dot_general(normed[...], forget_weight[...], NT, preferred_element_type=F32)
        + forget_bias[...]
    )
    forget_all = jnp.minimum(logits, 0.0) - jnp.log1p(jnp.exp(-jnp.abs(logits)))
    column = lax.broadcasted_iota(jnp.int32, forget_all.shape, 1)
    for index in range(heads):
        one = jnp.sum(
            jnp.where(column == me_tp * heads + index, forget_all, 0.0), axis=1, keepdims=True
        )
        forget_s[index] = jnp.broadcast_to(one, (rows, width))
    for copy in qkv_in:
        copy.wait()
    projected = jnp.dot(normed[...], qkv_v[...], preferred_element_type=F32).astype(BF16).astype(F32)
    query = projected[:, :width]
    key_new = projected[:, width : 2 * width]
    value_new = projected[:, 2 * width :]
    query_s[...] = query
    decay_in.wait()

    row16 = lax.broadcasted_iota(jnp.int32, (16, width), 0)
    lane16 = lax.broadcasted_iota(jnp.int32, (16, width), 1)
    head_mask = (lane16 < head) == (row16 < 8)
    row_in_group = lax.rem(row16, 8)
    lane8 = lax.broadcasted_iota(jnp.int32, (8, width), 1)

    @pl.loop(0, groups)
    def attend(group):
        eight = pl.ds(pl.multiple_of(group * 8, 8), 8)
        span = pl.ds(pl.multiple_of(group * group_depth, group_depth), group_depth)
        some = query_s[eight, :]
        both = jnp.where(head_mask, jnp.concatenate([some, some], axis=0), 0.0)
        spread = jnp.concatenate(
            [jnp.where(row_in_group == at, both, 0.0) for at in range(8)], axis=1
        ).astype(BF16)
        keys_copy(group).wait()
        scores = jnp.dot(spread, keys_v[span, :], preferred_element_type=F32) * scale
        extra = jnp.concatenate(
            [forget_s[0, eight, :][:, :1], forget_s[1, eight, :][:, :1]], axis=0
        )
        decay = jnp.concatenate([decay_v[eight, 0, :], decay_v[eight, 1, :]], axis=0)
        scores = scores + extra + decay
        top = jnp.max(scores, axis=1, keepdims=True)
        weight = jnp.exp(scores - top).astype(BF16)
        count = jnp.sum(weight.astype(F32), axis=1, keepdims=True)
        values_copy(group).wait()
        wide = lax.dot_general(weight, values_v[span, :], NT, preferred_element_type=F32)
        kept = jnp.zeros((16, width), F32)
        for at in range(8):
            kept = jnp.where(row_in_group == at, wide[:, at * width : (at + 1) * width], kept)
        low = lane8 < head
        parts[me_kv, 0, eight, :] = jnp.where(low, kept[:8], kept[8:])
        tops = jnp.where(low, top[:8], top[8:])
        counts = jnp.where(low, count[:8], count[8:])
        parts[me_kv, 1, eight, :] = jnp.where(lax.rem(lane8, head) < head // 2, tops, counts)

    copies = [send_kv(1, step, parts.at[me_kv], parts.at[me_kv]) for step in kv_order]
    lane = lax.broadcasted_iota(jnp.int32, (rows, width), 1)
    first = lane < head

    def per_head(low_column, high_column):
        return jnp.where(first, low_column, high_column)

    product = query * key_new
    own = (
        per_head(
            jnp.sum(jnp.where(first, product, 0.0), axis=1, keepdims=True),
            jnp.sum(jnp.where(first, 0.0, product), axis=1, keepdims=True),
        )
        * scale
    )
    arrive(copies)
    half = head // 2
    tops, counts, sums = [], [], []
    for block in range(n_kv):
        stat = parts[block, 1]
        sums.append(parts[block, 0])
        tops.append(per_head(stat[:, :1], stat[:, head : head + 1]))
        counts.append(per_head(stat[:, half : half + 1], stat[:, head + half : head + half + 1]))
    peak = functools.reduce(jnp.maximum, tops, own)
    factor = jnp.exp(own - peak)
    numer, denom = value_new * factor, factor
    for block in range(n_kv):
        factor = jnp.exp(tops[block] - peak)
        numer += sums[block] * factor
        denom += counts[block] * factor
    attention = (numer / denom).astype(BF16)

    out_in.wait()
    partial = jnp.dot(attention, out_v[...], preferred_element_type=F32)
    for piece in range(n_tp):
        out_parts[piece] = partial[:, piece * width : (piece + 1) * width]
    copies = [
        send_tp(1, step, out_parts.at[tp_peer(step)], out_got.at[me_tp]) for step in tp_order
    ]
    out_got[me_tp] = out_parts[me_tp]
    arrive(copies)
    total = out_got[0]
    for piece in range(1, n_tp):
        total += out_got[piece]
    middle = (pieces[me_kv, me_tp].astype(F32) + total).astype(BF16)
    middles[me_tp] = middle
    arrive([send_tp(2, step, middles.at[me_tp], middles.at[me_tp]) for step in tp_order])

    gains = channel_gain[pl.ds(pl.multiple_of(me_kv * n_tp, n_tp), n_tp), :]
    total = jnp.zeros((rows, width), F32)
    for piece in range(n_tp):
        wide = middles[piece].astype(F32)
        total += wide * wide
        mixed[:, piece * width : (piece + 1) * width] = (
            wide * gains[piece : piece + 1, :]
        ).astype(BF16)
    squares[me_kv] = jnp.broadcast_to(jnp.sum(total, axis=1, keepdims=True), (rows, width))
    copies = [send_kv(2, step, squares.at[me_kv], squares.at[me_kv]) for step in kv_order]
    up_in.wait()
    for step in kv_order + [0]:
        columns = pl.ds(pl.multiple_of(kv_peer(step) * chunk, chunk), chunk)
        partial = jnp.dot(mixed[...], up_v[:, columns], preferred_element_type=F32)
        if step:
            up_parts[step - 1] = partial
            copies.append(send_kv(3, step, up_parts.at[step - 1], up_got.at[me_kv]))
        else:
            up_got[me_kv] = partial
    arrive(copies)
    square = squares[0][:, :1]
    total = up_got[0]
    for block in range(1, n_kv):
        square += squares[block][:, :1]
        total += up_got[block]
    kept = jnp.maximum(total * lax.rsqrt(square / full + EPS), 0.0)
    hidden[me_kv] = (kept * kept).astype(BF16)
    copies = {step: send_kv(4, step, hidden.at[me_kv], hidden.at[me_kv]) for step in kv_order}
    down_in.wait()
    for at, step in enumerate([0] + list(range(1, n_kv))):
        source = lax.rem(me_kv + n_kv - step, n_kv)
        if step:
            copies[step].wait_recv()
        depth = pl.ds(pl.multiple_of(source * chunk, chunk), chunk)
        partial = jnp.dot(hidden[source], down_v[depth, :], preferred_element_type=F32)
        if at == 0:
            down_sum[...] = partial
        else:
            down_sum[...] += partial
    for piece in range(n_tp):
        down_parts[piece] = down_sum[:, piece * width : (piece + 1) * width]
    copies = [
        send_tp(3, step, down_parts.at[tp_peer(step)], down_got.at[me_tp]) for step in tp_order
    ]
    down_got[me_tp] = down_parts[me_tp]
    arrive(copies)
    total = down_got[0]
    for piece in range(1, n_tp):
        total += down_got[piece]
    result[...] = (middle.astype(F32) + total).astype(BF16)
    for copy in sent:
        copy.wait_send()


def fused_layer(
    stream,
    mixer_gain,
    query_weight,
    key_weight,
    value_weight,
    forget_weight,
    forget_bias,
    key_cache,
    value_cache,
    past_decay,
    out_weight,
    channel_gain,
    up_weight,
    down_weight,
):
    n_kv, n_tp = lax.axis_size("kv"), lax.axis_size("tp")
    rows, width = stream.shape
    _, heads, positions, head = key_cache.shape
    model, units = up_weight.shape
    chunk = units // n_kv
    columns = n_kv * n_tp
    sizes = (n_kv, n_tp, rows, width, chunk, heads, head)
    flat = rows * heads * head
    keys = jnp.transpose(key_cache, (0, 1, 3, 2)).reshape(flat, positions)
    values = jnp.transpose(value_cache, (0, 1, 3, 2)).reshape(flat, positions)
    in_vmem = pl.BlockSpec(memory_space=pltpu.VMEM)
    in_hbm = pl.BlockSpec(memory_space=pl.ANY)
    vmem = pltpu.VMEM
    dma = pltpu.SemaphoreType.DMA
    groups = rows // 8
    return pl.pallas_call(
        functools.partial(layer_kernel, sizes),
        out_shape=jax.ShapeDtypeStruct((rows, width), BF16),
        in_specs=[
            in_hbm, in_vmem, in_hbm, in_hbm, in_hbm, in_vmem, in_vmem,
            in_hbm, in_hbm, in_hbm, in_hbm, in_vmem, in_hbm, in_hbm,
        ],
        out_specs=in_vmem,
        scratch_shapes=[
            vmem((n_kv, n_tp, rows, width), BF16),
            vmem((columns * width, 3 * width), BF16),
            vmem((flat, positions), BF16),
            vmem((flat, positions), BF16),
            vmem(past_decay.shape, F32),
            vmem(out_weight.shape, BF16),
            vmem(up_weight.shape, BF16),
            vmem(down_weight.shape, BF16),
            vmem((rows, columns * width), BF16),
            vmem((rows, width), F32),
            vmem((heads, rows, width), F32),
            vmem((n_kv, 2, rows, width), F32),
            vmem((n_tp, rows, width), F32),
            vmem((n_tp, rows, width), F32),
            vmem((n_tp, rows, width), BF16),
            vmem((rows, model), BF16),
            vmem((n_kv, rows, width), F32),
            vmem((n_kv - 1, rows, chunk), F32),
            vmem((n_kv, rows, chunk), F32),
            vmem((n_kv, rows, chunk), BF16),
            vmem((rows, model), F32),
            vmem((n_tp, rows, width), F32),
            vmem((n_tp, rows, width), F32),
            dma((8,)),
            dma((groups,)),
            dma((groups,)),
            dma((4, n_tp - 1)),
            dma((4, n_tp - 1)),
            dma((5, n_kv - 1)),
            dma((5, n_kv - 1)),
        ],
        compiler_params=pltpu.CompilerParams(
            collective_id=0, has_side_effects=True, vmem_limit_bytes=60 * 1024 * 1024
        ),
    )(
        stream,
        mixer_gain.reshape(columns, width),
        query_weight,
        key_weight,
        value_weight,
        forget_weight.T,
        forget_bias.reshape(1, -1),
        keys,
        values,
        past_decay,
        out_weight,
        channel_gain.reshape(columns, width),
        up_weight,
        down_weight,
    )


def fits_kernel(mesh, stream, key_cache, up_weight):
    n_kv, n_tp = mesh.shape["kv"], mesh.shape["tp"]
    batch_rows, model = stream.shape
    heads, positions, head = key_cache.shape[1:]
    return (
        model // (n_kv * n_tp) == 128
        and heads // n_tp == 2
        and head == 64
        and batch_rows % 16 == 0
        and n_tp == 8
        and (positions // n_kv) % 128 == 0
        and (up_weight.shape[1] // (n_tp * n_kv)) % 128 == 0
    )


def solution(mesh):
    def layer(*arrays):
        local = fused_layer if fits_kernel(mesh, arrays[0], arrays[7], arrays[12]) else shards
        return run(local)(*arrays)

    def run(local):
        return jax.shard_map(
            local,
            mesh=mesh,
            in_specs=(
                P(None, ("kv", "tp")),
                P(),
                P(None, "tp"),
                P(None, "tp"),
                P(None, "tp"),
                P(),
                P(),
                P(None, "tp", "kv", None),
                P(None, "tp", "kv", None),
                P(None, "tp", "kv"),
                P("tp", "kv"),
                P(),
                P("kv", "tp"),
                P("tp", "kv"),
            ),
            out_specs=P(None, ("kv", "tp")),
            check_vma=False,
        )

    return layer
```
